32 devices in a mesh: dp: 4 (over y, x), kv: 4 (over z), tp: 2 (over core).
Axes of the slice: x: 2, y: 2, z: 4, core: 2. Of those that a mesh axis runs over, the one named last changes fastest.
Arguments:
- tokens: bfloat16 [4, 1024, 1024], P('dp', 'kv', 'tp'), may hold values from -6 to 6
- norm_gain: float32 [1024], replicated, may hold values from 0.1 to 1.9
- w_query: bfloat16 [1024, 1024], P(None, 'tp'), may hold values from -0.1875 to 0.1875
- w_key: bfloat16 [1024, 256], P(None, 'tp'), may hold values from -0.1875 to 0.1875
- w_value: bfloat16 [1024, 256], P(None, 'tp'), may hold values from -0.1875 to 0.1875
- q_gain: float32 [64], replicated, may hold values from 0.1 to 1.9
- k_gain: float32 [64], replicated, may hold values from 0.1 to 1.9
- w_out: bfloat16 [1024, 1024], P('tp'), may hold values from -4 to 4
- chosen: int32 [4, 32, 16], P('dp', 'kv'), may hold values from -1 to 31, as said below
Outputs:
- mixed: bfloat16 [4, 1024, 1024], P('dp', 'kv', 'tp')
- log_total: float32 [4, 16, 1024], P('dp', 'tp', 'kv')
The draws below stay inside these ranges and needn't reach their ends.
Inputs may be any that keep to these rules, and one draw needn't show every extreme that they name: Each row of chosen (one query block b) holds distinct key block numbers, all at most b, and -1 for empty entries; b itself is always present; a row is full (16 blocks) whenever at least 16 blocks may be chosen by it. Over the 8 rows of one index of kv, the chosen blocks that lie on any one other index of kv are at most 4 distinct ones, and exactly 4 of those on the index just before, for every index but the first. Some blocks are chosen far more often than others.
All inputs are finite; a program needn't handle non-finite values.
Results may differ from the reference program's by a relative error of at most 0.015.
Values may be sent and summed in bfloat16 or wider, within the bound.
A program may use at most 64 MiB of HBM per device.

```python
import jax
import jax.numpy as jnp
from jax import lax

D = 1024
H = 16
HD = 64
KVH = 4
BLK = 32
TOPB = 16
MOST = 4
NB_DEV = 8
NBLK = 32
SEQ = 1024
SEQS = 4
N_KV = 4


def chosen_sequence(seq_key):
    pop_key, cand_key, pick_key = jax.random.split(jax.random.fold_in(seq_key, 11), 3)
    block_ids = jnp.arange(NBLK, dtype=jnp.int32)
    owner_dev = block_ids // NB_DEV
    level_draw = jax.random.randint(pop_key, (NBLK,), 0, 4)
    appeal = level_draw * level_draw
    devices = jnp.arange(N_KV, dtype=jnp.int32)[:, None]
    noise_draw = jax.random.randint(cand_key, (N_KV, NBLK), 0, 1000)
    base_score = (appeal[None, :] * 1000 + noise_draw) * NBLK + block_ids[None, :]
    pinned = (block_ids[None, :] == devices * NB_DEV - 1) | (block_ids[None, :] == (devices - N_KV // 2) * NB_DEV)
    priority = jnp.where(pinned, base_score + 268435456, base_score).reshape(N_KV, N_KV, NB_DEV)
    threshold_val = lax.top_k(priority, MOST)[0][..., -1:]
    kept_set = (priority >= threshold_val).reshape(N_KV, NBLK)
    kept_set = jnp.where(owner_dev[None, :] == devices, True, kept_set & (owner_dev[None, :] < devices))
    query_ids = block_ids[:, None]
    row_dev = query_ids // NB_DEV
    candidate = kept_set[row_dev[:, 0]]
    allowed = candidate & (block_ids[None, :] <= query_ids)
    local_pos = query_ids % NB_DEV
    forced = (block_ids[None, :] == query_ids) | (block_ids[None, :] == query_ids - 1)
    forced = forced | (local_pos == 0) & (block_ids[None, :] == (row_dev - N_KV // 2) * NB_DEV)
    forced = forced | (local_pos == NB_DEV - 1) & candidate & (owner_dev[None, :] == row_dev - 1)
    second_noise = jax.random.randint(pick_key, (NBLK, NBLK), 0, 1000)
    ranking = (appeal[None, :] * 1000 + second_noise) * NBLK + block_ids[None, :]
    ranking = jnp.where(forced, ranking + 268435456, ranking)
    ranking = jnp.where(allowed, ranking, -1 - block_ids[None, :])
    top_vals, top_ids = lax.top_k(ranking, TOPB)
    return jnp.where(top_vals >= 0, top_ids, -1).astype(jnp.int32)


def draw_chosen(key, part):
    seq_keys = jax.random.split(jax.random.fold_in(key, 5), SEQS)
    return jax.vmap(chosen_sequence)(seq_keys)


def block_scale(key, dims, cuts, least, largest):
    factor_of = 1.0
    for position, parts in cuts:
        steps = jax.random.uniform(jax.random.fold_in(jax.random.fold_in(key, 6), position), (parts,), jnp.float32, least / len(cuts), largest / len(cuts))
        factor_of = factor_of * jnp.repeat(jnp.exp(steps), dims[position] // parts).reshape((-1,) + (1,) * (len(dims) - 1 - position))
    return factor_of


def gaussian(rng, extent, scale, bound, cuts=(), kind=jnp.bfloat16):
    entries = jax.random.normal(rng, extent, jnp.float32) * scale
    if len(cuts) > 0:
        entries = block_scale(rng, extent, cuts, -0.22, 0.18) * entries
    return jnp.clip(entries, min=-bound, max=bound).astype(kind)


def setup_inputs(seed: int = 0) -> dict:
    key_of = jax.random.split(jax.random.key(seed), 10)
    return {
        "tokens": gaussian(key_of[0], (SEQS, SEQ, D), 1.0, 6.0, ((0, 4), (1, 4), (2, 2))),
        "norm_gain": jnp.clip(1.0 + 0.18 * jax.random.normal(key_of[1], (D,), jnp.float32), 0.1, 1.9),
        "w_query": gaussian(key_of[2], (D, H * HD), D ** -0.5, 0.1875, ((1, 2),)),
        "w_key": gaussian(key_of[3], (D, KVH * HD), D ** -0.5, 0.1875, ((1, 2),)),
        "w_value": gaussian(key_of[4], (D, KVH * HD), D ** -0.5, 0.1875, ((1, 2),)),
        "q_gain": jnp.clip(1.0 + 0.18 * jax.random.normal(key_of[5], (HD,), jnp.float32), 0.1, 1.9),
        "k_gain": jnp.clip(1.0 + 0.18 * jax.random.normal(key_of[6], (HD,), jnp.float32), 0.1, 1.9),
        "w_out": gaussian(key_of[7], (H * HD, D), (8 * (H * HD) ** -0.5), 4.0, ((0, 2),)),
        "chosen": draw_chosen(jax.random.fold_in(key_of[9], 71), 0),
    }


epsilon = 1e-06
alibi_reach = 4.0

def rms_norm(values, gain):
    return values * lax.rsqrt(lax.optimization_barrier(jnp.mean(values * values, axis=-1, keepdims=True)) + epsilon) * gain.astype(jnp.float32)

def reference(tokens, norm_gain, w_query, w_key, w_value, q_gain, k_gain, w_out, chosen):
    group_size = H // KVH
    slopes = jnp.exp2(-8.0 * jnp.arange(1, H + 1, dtype=jnp.float32) / H)

    def one_sequence(seq_args):
        sequence_tokens, sequence_chosen = seq_args
        hidden = rms_norm(sequence_tokens.astype(jnp.float32), norm_gain).astype(jnp.bfloat16)
        queries = rms_norm(jnp.dot(hidden, w_query, preferred_element_type=jnp.float32).reshape(SEQ, H, HD), q_gain).astype(jnp.bfloat16)
        key_rows = rms_norm(jnp.dot(hidden, w_key, preferred_element_type=jnp.float32).reshape(SEQ, KVH, HD), k_gain).astype(jnp.bfloat16)
        value_rows = jnp.dot(hidden, w_value, preferred_element_type=jnp.float32).astype(jnp.bfloat16).reshape(SEQ, KVH, HD)
        key_blocks = key_rows.reshape(NBLK, BLK, KVH, HD)
        value_blocks = value_rows.reshape(NBLK, BLK, KVH, HD)

        def one_block(block_args):
            block_index, requested, query_block = block_args
            present = requested >= 0
            clamped = jnp.maximum(requested, 0).astype(jnp.int32)
            picked_keys = jnp.repeat(key_blocks[clamped].reshape(TOPB * BLK, KVH, HD), group_size, axis=1)
            picked_values = jnp.repeat(value_blocks[clamped].reshape(TOPB * BLK, KVH, HD), group_size, axis=1)
            scores = jnp.einsum('qhd,khd->hqk', query_block.astype(jnp.float32), picked_keys.astype(jnp.float32), precision=lax.Precision.HIGHEST) * HD ** (-0.5)
            query_pos = block_index * BLK + jnp.arange(BLK, dtype=jnp.int32)
            key_pos = (clamped[:, None] * BLK + jnp.arange(BLK, dtype=jnp.int32)[None, :]).reshape(-1)
            offset = (query_pos[:, None] - key_pos[None, :]).astype(jnp.float32)
            scores = scores - slopes[:, None, None] * offset[None] * alibi_reach / SEQ
            allowed = jnp.repeat(present, BLK)[None, :] & (offset >= 0)
            scores = jnp.where(allowed[None], scores, -jnp.inf)
            row_max = lax.optimization_barrier(jnp.max(scores, axis=-1, keepdims=True))
            weights = jnp.exp(scores - row_max)
            row_sum = lax.optimization_barrier(jnp.sum(weights, axis=-1, keepdims=True))
            block_log = row_max[..., 0] + jnp.log(row_sum[..., 0])
            probs = lax.optimization_barrier((weights / row_sum).astype(jnp.bfloat16))
            block_out = jnp.einsum('hqk,khd->qhd', probs.astype(jnp.float32), picked_values.astype(jnp.float32), precision=lax.Precision.HIGHEST)
            return (block_out, block_log)
        block_ids = jnp.arange(NBLK, dtype=jnp.int32)
        block_out, block_log = lax.map(one_block, (block_ids, sequence_chosen, queries.reshape(NBLK, BLK, H, HD)))
        attended = block_out.reshape(SEQ, H * HD).astype(jnp.bfloat16)
        mixed = jnp.dot(attended, w_out, preferred_element_type=jnp.float32).astype(jnp.bfloat16)
        log_total = block_log.transpose(1, 0, 2).reshape(H, SEQ)
        return (mixed, log_total)
    mixed, log_total = lax.map(one_sequence, (tokens, chosen))
    return (mixed, log_total)
```

```python
import functools
import math

import jax
import jax.numpy as jnp
from jax import lax
from jax.experimental import pallas as pl
from jax.experimental.pallas import tpu as pltpu
from jax.sharding import PartitionSpec as P

HD = 64
BLK = 32
MOST = 4
LANES = 128
PIECES = 3

epsilon = 1e-06
alibi_reach = 4.0
masked = -1e30
LOG2E = math.log2(math.e)
F32 = jnp.float32
BF16 = jnp.bfloat16
NT = (((1,), (1,)), ((), ()))


def iota(shape, dim):
    return lax.broadcasted_iota(jnp.int32, shape, dim)


def dot(a, b):
    return jnp.dot(a, b, preferred_element_type=F32)


def dot_nt(a, b):
    return lax.dot_general(a, b, NT, preferred_element_type=F32)


def kernel(
    n_kv,
    tok, gain, wq, wk, wv, qg, kg, wo, ch,
    out_ref, lt_ref,
    x_buf, ch_buf, w_buf, wo_buf, g_buf, qg_buf, kg_buf,
    q_s, kv_s, send_s, recv_s, acc, part_send, part_recv,
    load_sem, x_sem, ch_sem, kv_sem, part_sem,
):
    me = lax.axis_index("kv")
    tp = lax.axis_index("tp")
    partner = 1 - tp
    rows, half = tok.shape
    q_cols = wq.shape[1]
    k_cols = wk.shape[1]
    heads = q_cols // HD
    kv_heads = k_cols // HD
    group = heads // kv_heads
    n_heads = heads * lax.axis_size("tp")
    nb = ch.shape[0]
    entries = ch.shape[1]
    nbp = -(-n_kv * nb // LANES) * LANES
    picked = MOST * BLK
    width = half * 2
    seq_len = rows * n_kv
    alibi = alibi_reach / seq_len

    def span(start):
        return pl.ds(pl.multiple_of(start * half, LANES), half)

    loads = {}

    def load(name, pos, src, dst):
        copy = pltpu.make_async_copy(src, dst, load_sem.at[pos])
        copy.start()
        loads[name] = copy

    load("tok", 0, tok, x_buf.at[0])
    load("ch", 1, ch, ch_buf.at[me])
    load("g0", 2, gain.at[:, span(tp)], g_buf.at[0])
    load("g1", 3, gain.at[:, span(partner)], g_buf.at[1])
    load("qg", 4, qg, qg_buf)
    load("kg", 5, kg, kg_buf)
    for side, which in ((0, tp), (1, partner)):
        load(f"wq{side}", 6 + side, wq.at[span(which), :], w_buf.at[side, :, 0:q_cols])
        load(f"wk{side}", 8 + side, wk.at[span(which), :], w_buf.at[side, :, q_cols:q_cols + k_cols])
        load(f"wv{side}", 10 + side, wv.at[span(which), :], w_buf.at[side, :, q_cols + k_cols:q_cols + 2 * k_cols])
    for side, which in ((0, tp), (1, partner)):
        load(f"wo{side}", 12 + side, wo.at[:, span(which)], wo_buf.at[side])

    def peers(step):
        lax.fori_loop(1, n_kv, lambda d, c: (step(d), c)[1], 0, unroll=n_kv <= 8)

    barrier = pltpu.get_barrier_semaphore()
    pl.semaphore_signal(barrier, inc=1, device_id={"tp": partner}, device_id_type=pl.DeviceIdType.MESH)
    peers(lambda d: pl.semaphore_signal(
        barrier, inc=1, device_id={"kv": lax.rem(me + d, n_kv)}, device_id_type=pl.DeviceIdType.MESH))

    loads["tok"].wait()
    loads["ch"].wait()
    pl.semaphore_wait(barrier, n_kv)

    x_copy = pltpu.make_async_remote_copy(
        x_buf.at[0], x_buf.at[1], x_sem.at[0], x_sem.at[1],
        device_id={"tp": partner}, device_id_type=pl.DeviceIdType.MESH)
    x_copy.start()

    def list_copy(owner, target):
        return pltpu.make_async_remote_copy(
            ch_buf.at[owner], ch_buf.at[owner], ch_sem.at[0, target], ch_sem.at[1, owner],
            device_id={"kv": target}, device_id_type=pl.DeviceIdType.MESH)

    def send_list(d):
        @pl.when(me - d >= 0)
        def _():
            list_copy(me, lax.max(me - d, 0)).start()

    peers(send_list)

    def scaled(side):
        x = x_buf[side].astype(F32)
        return (x * g_buf[side]).astype(BF16), jnp.sum(x * x, axis=1, keepdims=True)

    for name in ("g0", "g1", "qg", "kg", "wq0", "wk0", "wv0"):
        loads[name].wait()
    y0, sq0 = scaled(0)
    raw = dot(y0, w_buf[0])
    for name in ("wq1", "wk1", "wv1"):
        loads[name].wait()
    x_copy.wait()
    y1, sq1 = scaled(1)
    raw = (raw + dot(y1, w_buf[1])) * lax.rsqrt((sq0 + sq1) / width + epsilon)

    same_head = jnp.where(
        iota((LANES, LANES), 0) // HD == iota((LANES, LANES), 1) // HD, 1.0, 0.0).astype(BF16)

    def head_norm(v, gain_row):
        sq = v * v
        hi = sq.astype(BF16)
        lo = (sq - hi.astype(F32)).astype(BF16)
        total = dot(hi, same_head) + dot(lo, same_head)
        return v * lax.rsqrt(total / HD + epsilon) * gain_row

    qg_row = jnp.concatenate([qg_buf[...], qg_buf[...]], axis=1) * (HD ** -0.5 * LOG2E)
    kg_row = jnp.concatenate([kg_buf[...], kg_buf[...]], axis=1)
    for tile in range(k_cols // LANES):
        at = tile * LANES
        kv_s[:, at:at + LANES] = head_norm(
            raw[:, q_cols + at:q_cols + at + LANES], kg_row).astype(BF16)
    kv_s[:, k_cols:] = raw[:, q_cols + k_cols:].astype(BF16)

    lane_block = iota((nb, nbp), 1)

    def member_of(lists):
        hit = lists[:, 0:1] == lane_block
        for e in range(1, entries):
            hit = hit | (lists[:, e:e + 1] == lane_block)
        return jnp.where(hit, 1.0, 0.0)

    before = jnp.where(
        (iota((nbp, nbp), 0) < iota((nbp, nbp), 1))
        & (iota((nbp, nbp), 0) // nb == iota((nbp, nbp), 1) // nb), 1.0, 0.0).astype(BF16)

    def need_and_rank(member):
        need = jnp.broadcast_to(jnp.max(member, axis=0, keepdims=True), (8, nbp))
        return need[0:1], dot(need.astype(BF16), before)[0:1]

    slot = (iota((picked, nbp), 0) // BLK).astype(F32)
    lane_owner = iota((picked, nbp), 1) // nb

    def one_hot(need, rank, owner):
        return jnp.where(
            (need > 0.5) & (rank == slot) & (lane_owner == owner), 1.0, 0.0).astype(BF16)

    spread = jnp.where(
        iota((nbp, rows), 0) == me * nb + iota((nbp, rows), 1) // BLK, 1.0, 0.0).astype(BF16)
    same_row = iota((picked, rows), 0) % BLK == iota((picked, rows), 1) % BLK

    def kv_copy(owner, target):
        return pltpu.make_async_remote_copy(
            send_s.at[target], recv_s.at[owner], kv_sem.at[0, target], kv_sem.at[1, owner],
            device_id={"kv": target}, device_id_type=pl.DeviceIdType.MESH)

    def send_rows(step):
        d = n_kv - step

        @pl.when(me + d < n_kv)
        def _():
            target = lax.min(me + d, n_kv - 1)
            list_copy(target, me).wait_recv()
            need, rank = need_and_rank(member_of(ch_buf[target]))
            chosen_rows = jnp.where(same_row, dot(one_hot(need, rank, me), spread), 0.0)
            send_s[target] = dot(chosen_rows.astype(BF16), kv_s[...]).astype(BF16)
            kv_copy(me, target).start()

    peers(send_rows)

    lane_q = iota((rows, LANES), 1)
    row_q = iota((rows, LANES), 0)
    own_block = jnp.where(lane_q - HD == row_q // BLK, 1.0, 0.0)

    def slope_of(head):
        return jnp.exp2(-8.0 / n_heads * (tp * heads + head + 1).astype(F32))

    def lane_fill(base, first, value):
        return jnp.where(lane_q == first, value, base)

    for tile in range(q_cols // LANES):
        at = tile * LANES
        q = head_norm(raw[:, at:at + LANES], qg_row)
        for odd in range(2):
            head = 2 * tile + odd
            value = slope_of(jnp.full((rows, LANES), head, jnp.int32)) * (alibi * LOG2E)
            extra = own_block
            for piece in range(PIECES):
                part = value.astype(BF16).astype(F32)
                value = value - part
                extra = lane_fill(extra, HD + nb + piece, part * BLK)
                extra = lane_fill(extra, HD + nb + PIECES + piece, part)
            here = q if odd == 0 else pltpu.roll(q, HD, 1)
            q_s[head] = jnp.where(lane_q < HD, here, extra).astype(BF16)

    member = member_of(ch_buf[me])
    relative = (lane_block - me * nb).astype(F32)
    pieces_rows = jnp.where(
        iota((8, nbp), 0) < PIECES,
        jnp.broadcast_to(relative[0:1], (8, nbp)), 0.0)
    table = jnp.concatenate(
        [jnp.zeros((HD, nbp), F32), member, pieces_rows,
         jnp.zeros((LANES - HD - nb - 8, nbp), F32)], axis=0).astype(BF16)

    def key_extra(hot):
        count = hot.shape[0]
        lane = iota((count, LANES), 1)
        found = dot_nt(hot, table)
        inside = (iota((count, LANES), 0) % BLK).astype(F32)
        tail = jnp.where(lane < HD + nb + 2 * PIECES, inside, 0.0)
        tail = jnp.where(lane < HD + nb + PIECES, found, tail)
        return jnp.where(lane < HD + nb, (found - 1.0) * -masked, tail)

    def attend(load_tile, extra, causal, first):
        count = extra.shape[0]
        low = iota((count, LANES), 1) < HD
        for g in range(kv_heads):
            at = g * HD // LANES * LANES
            k = load_tile(at).astype(F32)
            v = load_tile(k_cols + at).astype(F32)
            if g % 2:
                k = pltpu.roll(k, HD, 1)
                v = pltpu.roll(v, HD, 1)
            k = jnp.where(low, k, extra).astype(BF16)
            v = jnp.where(low, v, 1.0).astype(BF16)
            for h in range(g * group, (g + 1) * group):
                weights = jnp.exp2(dot_nt(q_s[h], k))
                if causal is not None:
                    weights = jnp.where(causal, weights, 0.0)
                add = dot(weights.astype(BF16), v)
                if first:
                    acc[h] = add
                else:
                    acc[h] += add

    hot_own = jnp.where(
        iota((rows, nbp), 1) == me * nb + iota((rows, nbp), 0) // BLK, 1.0, 0.0).astype(BF16)
    causal = iota((rows, rows), 1) <= iota((rows, rows), 0)
    attend(lambda at: kv_s[:, at:at + LANES], key_extra(hot_own), causal, True)

    need_own, rank_own = need_and_rank(member)

    def absorb(d):
        @pl.when(me - d >= 0)
        def _():
            owner = lax.max(me - d, 0)
            extra = key_extra(one_hot(need_own, rank_own, owner))
            kv_copy(owner, me).wait_recv()
            attend(lambda at: recv_s[owner, :, at:at + LANES], extra, None, False)

    peers(absorb)

    sums = jnp.ones((rows, LANES), F32)
    tiles = []
    for tile in range(q_cols // LANES):
        sides = []
        for odd in range(2):
            head = 2 * tile + odd
            o = acc[head]
            total = pltpu.roll(o, HD, 1)
            sums = jnp.where(lane_q == head, total, sums)
            sides.append(o / total)
        tiles.append(jnp.where(lane_q < HD, sides[0], pltpu.roll(sides[1], HD, 1)))
    attended = jnp.concatenate(tiles, axis=1).astype(BF16)

    loads["wo1"].wait()
    part_send[...] = dot(attended, wo_buf[1]).astype(BF16)
    part_copy = pltpu.make_async_remote_copy(
        part_send, part_recv, part_sem.at[0], part_sem.at[1],
        device_id={"tp": partner}, device_id_type=pl.DeviceIdType.MESH)
    part_copy.start()
    loads["wo0"].wait()
    own = dot(attended, wo_buf[0])
    logs = jnp.log(sums) - slope_of(lane_q) * alibi * row_q.astype(F32)
    lt_ref[...] = logs.T[0:heads]

    def finish(d):
        @pl.when(me + d < n_kv)
        def _():
            kv_copy(me, lax.min(me + d, n_kv - 1)).wait_send()

        @pl.when(me - d >= 0)
        def _():
            list_copy(me, lax.max(me - d, 0)).wait_send()

    peers(finish)
    part_copy.wait()
    out_ref[...] = (own + part_recv[...].astype(F32)).astype(BF16)


def shards(n_kv, tokens, norm_gain, w_query, w_key, w_value, q_gain, k_gain, w_out, chosen):
    seqs, rows, half = tokens.shape
    nb, entries = chosen.shape[1:]
    q_cols, k_cols = w_query.shape[1], w_key.shape[1]
    heads = q_cols // HD
    vmem = pltpu.VMEM
    dma = pltpu.SemaphoreType.DMA
    mixed, log_total = pl.pallas_call(
        functools.partial(kernel, n_kv),
        out_shape=(
            jax.ShapeDtypeStruct((rows, half), BF16),
            jax.ShapeDtypeStruct((heads, rows), F32),
        ),
        in_specs=[pl.BlockSpec(memory_space=pl.ANY)] * 9,
        out_specs=(pl.BlockSpec(memory_space=vmem), pl.BlockSpec(memory_space=vmem)),
        scratch_shapes=[
            vmem((2, rows, half), BF16),
            vmem((n_kv, nb, entries), jnp.int32),
            vmem((2, half, q_cols + 2 * k_cols), BF16),
            vmem((2, q_cols, half), BF16),
            vmem((2, 1, half), F32),
            vmem((1, HD), F32),
            vmem((1, HD), F32),
            vmem((heads, rows, LANES), BF16),
            vmem((rows, 2 * k_cols), BF16),
            vmem((n_kv, MOST * BLK, 2 * k_cols), BF16),
            vmem((n_kv, MOST * BLK, 2 * k_cols), BF16),
            vmem((heads, rows, LANES), F32),
            vmem((rows, half), BF16),
            vmem((rows, half), BF16),
            dma((14,)),
            dma((2,)),
            dma((2, n_kv)),
            dma((2, n_kv)),
            dma((2,)),
        ],
        compiler_params=pltpu.CompilerParams(
            collective_id=0, has_side_effects=True, vmem_limit_bytes=48 * 1024 * 1024
        ),
    )(
        tokens.reshape(rows, half), norm_gain.reshape(1, -1), w_query, w_key, w_value,
        q_gain.reshape(1, -1), k_gain.reshape(1, -1), w_out, chosen.reshape(nb, entries),
    )
    return mixed.reshape(seqs, rows, half), log_total.reshape(seqs, heads, rows)


def solution(mesh):
    in_specs = (
        P("dp", "kv", "tp"),
        P(),
        P(None, "tp"),
        P(None, "tp"),
        P(None, "tp"),
        P(),
        P(),
        P("tp", None),
        P("dp", "kv", None),
    )
    out_specs = (P("dp", "kv", "tp"), P("dp", "tp", "kv"))
    return jax.shard_map(
        functools.partial(shards, mesh.shape["kv"]),
        mesh=mesh, in_specs=in_specs, out_specs=out_specs, check_vma=False)
```

```python
import functools
import math

import jax
import jax.numpy as jnp
from jax import lax
from jax.experimental import pallas as pl
from jax.experimental.pallas import tpu as pltpu
from jax.sharding import PartitionSpec as P

HD = 64
BLK = 32
MOST = 4
LANES = 128
PIECES = 3

epsilon = 1e-06
alibi_reach = 4.0
masked = -1e30
LOG2E = math.log2(math.e)
F32 = jnp.float32
BF16 = jnp.bfloat16
NT = (((1,), (1,)), ((), ()))


def iota(shape, dim):
    return lax.broadcasted_iota(jnp.int32, shape, dim)


def dot(a, b):
    return jnp.dot(a, b, preferred_element_type=F32)


def dot_nt(a, b):
    return lax.dot_general(a, b, NT, preferred_element_type=F32)


def kernel(
    n_kv,
    tok, gain, wq, wk, wv, qg, kg, wo, ch,
    out_ref, lt_ref,
    x_buf, ch_buf, w_buf, wo_buf, g_buf, qg_buf, kg_buf,
    q_s, kv_s, send_s, recv_s, acc, part_send, part_recv,
    load_sem, x_sem, ch_sem, kv_sem, part_sem,
):
    me = lax.axis_index("kv")
    tp = lax.axis_index("tp")
    partner = 1 - tp
    rows, half = tok.shape
    q_cols = wq.shape[1]
    k_cols = wk.shape[1]
    heads = q_cols // HD
    kv_heads = k_cols // HD
    group = heads // kv_heads
    n_heads = heads * lax.axis_size("tp")
    nb = ch.shape[0]
    entries = ch.shape[1]
    nbp = -(-n_kv * nb // LANES) * LANES
    picked = MOST * BLK
    width = half * 2
    seq_len = rows * n_kv
    alibi = alibi_reach / seq_len

    def span(start):
        return pl.ds(pl.multiple_of(start * half, LANES), half)

    loads = {}

    def load(name, pos, src, dst):
        copy = pltpu.make_async_copy(src, dst, load_sem.at[pos])
        copy.start()
        loads[name] = copy

    load("tok", 0, tok, x_buf.at[0])
    load("ch", 1, ch, ch_buf.at[me])
    load("g0", 2, gain.at[:, span(tp)], g_buf.at[0])
    load("g1", 3, gain.at[:, span(partner)], g_buf.at[1])
    load("qg", 4, qg, qg_buf)
    load("kg", 5, kg, kg_buf)
    for side, which in ((0, tp), (1, partner)):
        load(f"wq{side}", 6 + side, wq.at[span(which), :], w_buf.at[side, :, 0:q_cols])
        load(f"wk{side}", 8 + side, wk.at[span(which), :], w_buf.at[side, :, q_cols:q_cols + k_cols])
        load(f"wv{side}", 10 + side, wv.at[span(which), :], w_buf.at[side, :, q_cols + k_cols:q_cols + 2 * k_cols])
    for side, which in ((0, tp), (1, partner)):
        load(f"wo{side}", 12 + side, wo.at[:, span(which)], wo_buf.at[side])

    def peers(step):
        lax.fori_loop(1, n_kv, lambda d, c: (step(d), c)[1], 0, unroll=n_kv <= 8)

    barrier = pltpu.get_barrier_semaphore()
    pl.semaphore_signal(barrier, inc=1, device_id={"tp": partner}, device_id_type=pl.DeviceIdType.MESH)
    peers(lambda d: pl.semaphore_signal(
        barrier, inc=1, device_id={"kv": lax.rem(me + d, n_kv)}, device_id_type=pl.DeviceIdType.MESH))

    loads["tok"].wait()
    loads["ch"].wait()
    pl.semaphore_wait(barrier, n_kv)

    x_copy = pltpu.make_async_remote_copy(
        x_buf.at[0], x_buf.at[1], x_sem.at[0], x_sem.at[1],
        device_id={"tp": partner}, device_id_type=pl.DeviceIdType.MESH)
    x_copy.start()

    def list_copy(owner, target):
        return pltpu.make_async_remote_copy(
            ch_buf.at[owner], ch_buf.at[owner], ch_sem.at[0, target], ch_sem.at[1, owner],
            device_id={"kv": target}, device_id_type=pl.DeviceIdType.MESH)

    def send_list(d):
        @pl.when(me - d >= 0)
        def _():
            list_copy(me, lax.max(me - d, 0)).start()

    peers(send_list)

    def scaled(side):
        x = x_buf[side].astype(F32)
        return (x * g_buf[side]).astype(BF16), jnp.sum(x * x, axis=1, keepdims=True)

    for name in ("g0", "g1", "qg", "kg", "wq0", "wk0", "wv0"):
        loads[name].wait()
    y0, sq0 = scaled(0)
    raw = dot(y0, w_buf[0])
    for name in ("wq1", "wk1", "wv1"):
        loads[name].wait()
    x_copy.wait()
    y1, sq1 = scaled(1)
    raw = (raw + dot(y1, w_buf[1])) * lax.rsqrt((sq0 + sq1) / width + epsilon)

    same_head = jnp.where(
        iota((LANES, LANES), 0) // HD == iota((LANES, LANES), 1) // HD, 1.0, 0.0).astype(BF16)

    def head_norm(v, gain_row):
        sq = v * v
        hi = sq.astype(BF16)
        lo = (sq - hi.astype(F32)).astype(BF16)
        total = dot(hi, same_head) + dot(lo, same_head)
        return v * lax.rsqrt(total / HD + epsilon) * gain_row

    qg_row = jnp.concatenate([qg_buf[...], qg_buf[...]], axis=1) * (HD ** -0.5 * LOG2E)
    kg_row = jnp.concatenate([kg_buf[...], kg_buf[...]], axis=1)
    for tile in range(k_cols // LANES):
        at = tile * LANES
        kv_s[:, at:at + LANES] = head_norm(
            raw[:, q_cols + at:q_cols + at + LANES], kg_row).astype(BF16)
    kv_s[:, k_cols:] = raw[:, q_cols + k_cols:].astype(BF16)

    lane_block = iota((nb, nbp), 1)

    def member_of(lists):
        hit = lists[:, 0:1] == lane_block
        for e in range(1, entries):
            hit = hit | (lists[:, e:e + 1] == lane_block)
        return jnp.where(hit, 1.0, 0.0)

    before = jnp.where(
        (iota((nbp, nbp), 0) < iota((nbp, nbp), 1))
        & (iota((nbp, nbp), 0) // nb == iota((nbp, nbp), 1) // nb), 1.0, 0.0).astype(BF16)

    def need_and_rank(member):
        need = jnp.broadcast_to(jnp.max(member, axis=0, keepdims=True), (8, nbp))
        return need[0:1], dot(need.astype(BF16), before)[0:1]

    slot = (iota((picked, nbp), 0) // BLK).astype(F32)
    lane_owner = iota((picked, nbp), 1) // nb

    def one_hot(need, rank, owner):
        return jnp.where(
            (need > 0.5) & (rank == slot) & (lane_owner == owner), 1.0, 0.0).astype(BF16)

    spread = jnp.where(
        iota((nbp, rows), 0) == me * nb + iota((nbp, rows), 1) // BLK, 1.0, 0.0).astype(BF16)
    same_row = iota((picked, rows), 0) % BLK == iota((picked, rows), 1) % BLK

    def kv_copy(owner, target):
        return pltpu.make_async_remote_copy(
            send_s.at[target], recv_s.at[owner], kv_sem.at[0, target], kv_sem.at[1, owner],
            device_id={"kv": target}, device_id_type=pl.DeviceIdType.MESH)

    def send_rows(step):
        d = n_kv - step

        @pl.when(me + d < n_kv)
        def _():
            target = lax.min(me + d, n_kv - 1)
            list_copy(target, me).wait_recv()
            need, rank = need_and_rank(member_of(ch_buf[target]))
            chosen_rows = jnp.where(same_row, dot(one_hot(need, rank, me), spread), 0.0)
            send_s[target] = dot(chosen_rows.astype(BF16), kv_s[...]).astype(BF16)
            kv_copy(me, target).start()

    peers(send_rows)

    lane_q = iota((rows, LANES), 1)
    row_q = iota((rows, LANES), 0)
    own_block = jnp.where(lane_q - HD == row_q // BLK, 1.0, 0.0)

    def slope_of(head):
        return jnp.exp2(-8.0 / n_heads * (tp * heads + head + 1).astype(F32))

    def lane_fill(base, first, value):
        return jnp.where(lane_q == first, value, base)

    for tile in range(q_cols // LANES):
        at = tile * LANES
        q = head_norm(raw[:, at:at + LANES], qg_row)
        for odd in range(2):
            head = 2 * tile + odd
            value = slope_of(jnp.full((rows, LANES), head, jnp.int32)) * (alibi * LOG2E)
            extra = own_block
            for piece in range(PIECES):
                part = value.astype(BF16).astype(F32)
                value = value - part
                extra = lane_fill(extra, HD + nb + piece, part * BLK)
                extra = lane_fill(extra, HD + nb + PIECES + piece, part)
            here = q if odd == 0 else pltpu.roll(q, HD, 1)
            q_s[head] = jnp.where(lane_q < HD, here, extra).astype(BF16)

    member = member_of(ch_buf[me])
    relative = (lane_block - me * nb).astype(F32)
    pieces_rows = jnp.where(
        iota((8, nbp), 0) < PIECES,
        jnp.broadcast_to(relative[0:1], (8, nbp)), 0.0)
    table = jnp.concatenate(
        [jnp.zeros((HD, nbp), F32), member, pieces_rows,
         jnp.zeros((LANES - HD - nb - 8, nbp), F32)], axis=0).astype(BF16)

    def key_extra(hot):
        count = hot.shape[0]
        lane = iota((count, LANES), 1)
        found = dot_nt(hot, table)
        inside = (iota((count, LANES), 0) % BLK).astype(F32)
        tail = jnp.where(lane < HD + nb + 2 * PIECES, inside, 0.0)
        tail = jnp.where(lane < HD + nb + PIECES, found, tail)
        return jnp.where(lane < HD + nb, (found - 1.0) * -masked, tail)

    def attend(load_tile, extra, causal, first):
        count = extra.shape[0]
        low = iota((count, LANES), 1) < HD
        for g in range(kv_heads):
            at = g * HD // LANES * LANES
            k = load_tile(at).astype(F32)
            v = load_tile(k_cols + at).astype(F32)
            if g % 2:
                k = pltpu.roll(k, HD, 1)
                v = pltpu.roll(v, HD, 1)
            k = jnp.where(low, k, extra).astype(BF16)
            v = jnp.where(low, v, 1.0).astype(BF16)
            for h in range(g * group, (g + 1) * group):
                weights = jnp.exp2(dot_nt(q_s[h], k))
                if causal is not None:
                    weights = jnp.where(causal, weights, 0.0)
                add = dot(weights.astype(BF16), v)
                if first:
                    acc[h] = add
                else:
                    acc[h] += add

    hot_own = jnp.where(
        iota((rows, nbp), 1) == me * nb + iota((rows, nbp), 0) // BLK, 1.0, 0.0).astype(BF16)
    causal = iota((rows, rows), 1) <= iota((rows, rows), 0)
    attend(lambda at: kv_s[:, at:at + LANES], key_extra(hot_own), causal, True)

    need_own, rank_own = need_and_rank(member)

    def absorb(d):
        @pl.when(me - d >= 0)
        def _():
            owner = lax.max(me - d, 0)
            extra = key_extra(one_hot(need_own, rank_own, owner))
            kv_copy(owner, me).wait_recv()
            attend(lambda at: recv_s[owner, :, at:at + LANES], extra, None, False)

    peers(absorb)

    sums = jnp.ones((rows, LANES), F32)
    tiles = []
    for tile in range(q_cols // LANES):
        sides = []
        for odd in range(2):
            head = 2 * tile + odd
            o = acc[head]
            total = pltpu.roll(o, HD, 1)
            sums = jnp.where(lane_q == head, total, sums)
            sides.append(o / total)
        tiles.append(jnp.where(lane_q < HD, sides[0], pltpu.roll(sides[1], HD, 1)))
    attended = jnp.concatenate(tiles, axis=1).astype(BF16)

    loads["wo1"].wait()
    part_send[...] = dot(attended, wo_buf[1]).astype(BF16)
    part_copy = pltpu.make_async_remote_copy(
        part_send, part_recv, part_sem.at[0], part_sem.at[1],
        device_id={"tp": partner}, device_id_type=pl.DeviceIdType.MESH)
    part_copy.start()
    loads["wo0"].wait()
    own = dot(attended, wo_buf[0])
    logs = jnp.log(sums) - slope_of(lane_q) * alibi * row_q.astype(F32)
    lt_ref[...] = logs.T[0:heads]

    def finish(d):
        @pl.when(me + d < n_kv)
        def _():
            kv_copy(me, lax.min(me + d, n_kv - 1)).wait_send()

        @pl.when(me - d >= 0)
        def _():
            list_copy(me, lax.max(me - d, 0)).wait_send()

    peers(finish)
    part_copy.wait()
    out_ref[...] = (own + part_recv[...].astype(F32)).astype(BF16)


def write_out(mixed, log_total, mixed_out, log_out, sems):
    copies = [
        pltpu.make_async_copy(mixed, mixed_out, sems.at[0]),
        pltpu.make_async_copy(log_total, log_out, sems.at[1]),
    ]
    for copy in copies:
        copy.start()
    for copy in copies:
        copy.wait()


def shards(n_kv, tokens, norm_gain, w_query, w_key, w_value, q_gain, k_gain, w_out, chosen):
    seqs, rows, half = tokens.shape
    nb, entries = chosen.shape[1:]
    q_cols, k_cols = w_query.shape[1], w_key.shape[1]
    heads = q_cols // HD
    vmem = pltpu.VMEM
    dma = pltpu.SemaphoreType.DMA
    mixed, log_total = pl.pallas_call(
        functools.partial(kernel, n_kv),
        out_shape=(
            jax.ShapeDtypeStruct((rows, half), BF16),
            jax.ShapeDtypeStruct((heads, rows), F32),
        ),
        in_specs=[pl.BlockSpec(memory_space=pltpu.HBM)] * 9,
        out_specs=(pl.BlockSpec(memory_space=vmem), pl.BlockSpec(memory_space=vmem)),
        scratch_shapes=[
            vmem((2, rows, half), BF16),
            vmem((n_kv, nb, entries), jnp.int32),
            vmem((2, half, q_cols + 2 * k_cols), BF16),
            vmem((2, q_cols, half), BF16),
            vmem((2, 1, half), F32),
            vmem((1, HD), F32),
            vmem((1, HD), F32),
            vmem((heads, rows, LANES), BF16),
            vmem((rows, 2 * k_cols), BF16),
            vmem((n_kv, MOST * BLK, 2 * k_cols), BF16),
            vmem((n_kv, MOST * BLK, 2 * k_cols), BF16),
            vmem((heads, rows, LANES), F32),
            vmem((rows, half), BF16),
            vmem((rows, half), BF16),
            dma((14,)),
            dma((2,)),
            dma((2, n_kv)),
            dma((2, n_kv)),
            dma((2,)),
        ],
        compiler_params=pltpu.CompilerParams(
            collective_id=0, has_side_effects=True, vmem_limit_bytes=66_000_000
        ),
    )(
        tokens.reshape(rows, half), norm_gain.reshape(1, -1), w_query, w_key, w_value,
        q_gain.reshape(1, -1), k_gain.reshape(1, -1), w_out, chosen.reshape(nb, entries),
    )
    mixed, log_total = pl.pallas_call(
        write_out,
        out_shape=(
            jax.ShapeDtypeStruct((rows, half), BF16),
            jax.ShapeDtypeStruct((heads, rows), F32),
        ),
        in_specs=[pl.BlockSpec(memory_space=vmem)] * 2,
        out_specs=(pl.BlockSpec(memory_space=pltpu.HBM),) * 2,
        scratch_shapes=[dma((2,))],
    )(mixed, log_total)
    return mixed.reshape(seqs, rows, half), log_total.reshape(seqs, heads, rows)


def solution(mesh):
    in_specs = (
        P("dp", "kv", "tp"),
        P(),
        P(None, "tp"),
        P(None, "tp"),
        P(None, "tp"),
        P(),
        P(),
        P("tp", None),
        P("dp", "kv", None),
    )
    out_specs = (P("dp", "kv", "tp"), P("dp", "tp", "kv"))
    return jax.shard_map(
        functools.partial(shards, mesh.shape["kv"]),
        mesh=mesh, in_specs=in_specs, out_specs=out_specs, check_vma=False)
```

```python
import functools
import math

import jax
import jax.numpy as jnp
from jax import lax
from jax.experimental import pallas as pl
from jax.experimental.pallas import tpu as pltpu
from jax.sharding import PartitionSpec as P

HD = 64
BLK = 32
MOST = 4
LANES = 128
PIECES = 3
PARTS = 2

epsilon = 1e-06
alibi_reach = 4.0
masked = -1e30
LOG2E = math.log2(math.e)
F32 = jnp.float32
BF16 = jnp.bfloat16
NT = (((1,), (1,)), ((), ()))


def iota(shape, dim):
    return lax.broadcasted_iota(jnp.int32, shape, dim)


def dot(a, b):
    return jnp.dot(a, b, preferred_element_type=F32)


def dot_nt(a, b):
    return lax.dot_general(a, b, NT, preferred_element_type=F32)


def kernel(
    n_kv,
    tok, gain, wq, wk, wv, qg, kg, wo, ch,
    out_ref, lt_ref,
    x_buf, ch_buf, code_send, code_recv, raw_s, w_buf, wo_buf, g_buf, qg_buf, kg_buf,
    q_s, kv_s, send_s, recv_s, acc, part_send, part_recv,
    load_sem, x_sem, ch_sem, kv_sem, part_sem,
):
    me = lax.axis_index("kv")
    tp = lax.axis_index("tp")
    partner = 1 - tp
    rows, half = tok.shape
    q_cols = wq.shape[1]
    k_cols = wk.shape[1]
    heads = q_cols // HD
    kv_heads = k_cols // HD
    group = heads // kv_heads
    n_heads = heads * lax.axis_size("tp")
    nb = ch.shape[0]
    entries = ch.shape[1]
    nbp = -(-n_kv * nb // LANES) * LANES
    picked = MOST * BLK
    width = half * 2
    seq_len = rows * n_kv
    alibi = alibi_reach / seq_len

    def span(start):
        return pl.ds(pl.multiple_of(start * half, LANES), half)

    loads = {}

    def load(name, src, dst):
        copy = pltpu.make_async_copy(src, dst, load_sem.at[len(loads)])
        copy.start()
        loads[name] = copy

    sides = ((0, tp), (1, partner))
    load("ch", ch, ch_buf)
    load("tok", tok, x_buf.at[0])
    load("g0", gain.at[:, span(tp)], g_buf.at[0])
    for side, which in sides:
        load(f"wk{side}", wk.at[span(which), :], w_buf.at[side, :, q_cols:q_cols + k_cols])
        load(f"wv{side}", wv.at[span(which), :], w_buf.at[side, :, q_cols + k_cols:q_cols + 2 * k_cols])
        load(f"wq{side}", wq.at[span(which), :], w_buf.at[side, :, 0:q_cols])
    load("g1", gain.at[:, span(partner)], g_buf.at[1])
    load("qg", qg, qg_buf)
    load("kg", kg, kg_buf)
    for side, which in sides:
        load(f"wo{side}", wo.at[:, span(which)], wo_buf.at[side])

    def peers(step):
        if n_kv <= 8:
            for d in range(1, n_kv):
                step(d)
        else:
            lax.fori_loop(1, n_kv, lambda d, c: (step(d), c)[1], 0)

    barrier = pltpu.get_barrier_semaphore()
    pl.semaphore_signal(barrier, inc=1, device_id={"tp": partner}, device_id_type=pl.DeviceIdType.MESH)
    peers(lambda d: pl.semaphore_signal(
        barrier, inc=1, device_id={"kv": lax.rem(me + d, n_kv)}, device_id_type=pl.DeviceIdType.MESH))

    loads["ch"].wait()
    lane_block = iota((nb, nbp), 1)
    lists = ch_buf[...]
    hit = lists[:, 0:1] == lane_block
    for e in range(1, entries):
        hit = hit | (lists[:, e:e + 1] == lane_block)
    member = jnp.where(hit, 1.0, 0.0)
    before = jnp.where(
        (iota((nbp, nbp), 0) < iota((nbp, nbp), 1))
        & (iota((nbp, nbp), 0) // nb == iota((nbp, nbp), 1) // nb), 1.0, 0.0).astype(BF16)
    need = jnp.broadcast_to(jnp.max(member, axis=0, keepdims=True), (8, nbp))
    place = jnp.where(need > 0.5, dot(need.astype(BF16), before), -1.0)

    def place_rows(owner):
        spread = jnp.where(
            iota((nbp, rows), 0) == owner * nb + iota((nbp, rows), 1) // BLK, 1.0, 0.0)
        return dot(place.astype(BF16), spread.astype(BF16))

    code_recv[me] = place_rows(me)

    def prepare_code(d):
        code_send[d] = place_rows(me - d)

    peers(prepare_code)

    def scaled(side):
        x = x_buf[side].astype(F32)
        return (x * g_buf[side]).astype(BF16), jnp.sum(x * x, axis=1, keepdims=True)

    for name in ("tok", "g0", "wk0", "wv0", "wq0"):
        loads[name].wait()
    y0, sq0 = scaled(0)
    raw_s[...] = dot(y0, w_buf[0])
    pl.semaphore_wait(barrier, n_kv)

    x_copy = pltpu.make_async_remote_copy(
        x_buf.at[0], x_buf.at[1], x_sem.at[0], x_sem.at[1],
        device_id={"tp": partner}, device_id_type=pl.DeviceIdType.MESH)
    x_copy.start()

    def code_copy(owner, target, d):
        return pltpu.make_async_remote_copy(
            code_send.at[d], code_recv.at[owner], ch_sem.at[0, target], ch_sem.at[1, owner],
            device_id={"kv": target}, device_id_type=pl.DeviceIdType.MESH)

    def send_code(d):
        @pl.when(me - d >= 0)
        def _():
            code_copy(me, lax.max(me - d, 0), d).start()

    peers(send_code)

    same_head = jnp.where(
        iota((LANES, LANES), 0) // HD == iota((LANES, LANES), 1) // HD, 1.0, 0.0).astype(BF16)

    def head_norm(v, gain_row):
        sq = v * v
        hi = sq.astype(BF16)
        lo = (sq - hi.astype(F32)).astype(BF16)
        total = dot(hi, same_head) + dot(lo, same_head)
        return v * lax.rsqrt(total / HD + epsilon) * gain_row

    for name in ("g1", "qg", "kg", "wk1", "wv1", "wq1"):
        loads[name].wait()
    qg_row = jnp.concatenate([qg_buf[...], qg_buf[...]], axis=1) * (HD ** -0.5 * LOG2E)
    kg_row = jnp.concatenate([kg_buf[...], kg_buf[...]], axis=1)
    x_copy.wait()
    y1, sq1 = scaled(1)
    row_scale = lax.rsqrt((sq0 + sq1) / width + epsilon)
    raw_kv = (raw_s[:, q_cols:] + dot(y1, w_buf[1, :, q_cols:])) * row_scale
    for tile in range(k_cols // LANES):
        at = tile * LANES
        kv_s[:, at:at + LANES] = head_norm(raw_kv[:, at:at + LANES], kg_row).astype(BF16)
    kv_s[:, k_cols:] = raw_kv[:, k_cols:].astype(BF16)

    same_row = iota((picked, rows), 0) % BLK == iota((picked, rows), 1) % BLK
    row_slot = (iota((picked, rows), 0) // BLK).astype(F32)

    def kv_copy(owner, target, d):
        return pltpu.make_async_remote_copy(
            send_s.at[d], recv_s.at[owner], kv_sem.at[0, target], kv_sem.at[1, owner],
            device_id={"kv": target}, device_id_type=pl.DeviceIdType.MESH)

    def await_code(d):
        @pl.when(me + d < n_kv)
        def _():
            code_copy(lax.min(me + d, n_kv - 1), me, d).wait_recv()

    def pack(d):
        code = code_recv[lax.min(me + d, n_kv - 1)][0:1]
        chosen_rows = jnp.where(same_row & (code == row_slot), 1.0, 0.0).astype(BF16)
        send_s[d] = dot(chosen_rows, kv_s[...]).astype(BF16)

    def send_rows(step):
        d = n_kv - step

        @pl.when(me + d < n_kv)
        def _():
            kv_copy(me, lax.min(me + d, n_kv - 1), d).start()

    peers(await_code)
    peers(pack)
    peers(send_rows)
    raw = (raw_s[:, 0:q_cols] + dot(y1, w_buf[1, :, 0:q_cols])) * row_scale

    lane_q = iota((rows, LANES), 1)
    row_q = iota((rows, LANES), 0)
    own_block = jnp.where(lane_q - HD == row_q // BLK, 1.0, 0.0)

    def slope_of(head):
        return jnp.exp2(-8.0 / n_heads * (tp * heads + head + 1).astype(F32))

    def lane_fill(base, first, value):
        return jnp.where(lane_q == first, value, base)

    for tile in range(q_cols // LANES):
        at = tile * LANES
        q = head_norm(raw[:, at:at + LANES], qg_row)
        for odd in range(2):
            head = 2 * tile + odd
            value = slope_of(jnp.full((rows, LANES), head, jnp.int32)) * (alibi * LOG2E)
            extra = own_block
            for piece in range(PIECES):
                part = value.astype(BF16).astype(F32)
                value = value - part
                extra = lane_fill(extra, HD + nb + piece, part * BLK)
                extra = lane_fill(extra, HD + nb + PIECES + piece, part)
            here = q if odd == 0 else pltpu.roll(q, HD, 1)
            q_s[head] = jnp.where(lane_q < HD, here, extra).astype(BF16)

    relative = (lane_block - me * nb).astype(F32)
    pieces_rows = jnp.where(
        iota((8, nbp), 0) < PIECES,
        jnp.broadcast_to(relative[0:1], (8, nbp)), 0.0)
    table = jnp.concatenate(
        [jnp.zeros((HD, nbp), F32), member, pieces_rows,
         jnp.zeros((LANES - HD - nb - 8, nbp), F32)], axis=0).astype(BF16)

    def key_extra(hot):
        count = hot.shape[0]
        lane = iota((count, LANES), 1)
        found = dot_nt(hot, table)
        inside = (iota((count, LANES), 0) % BLK).astype(F32)
        tail = jnp.where(lane < HD + nb + 2 * PIECES, inside, 0.0)
        tail = jnp.where(lane < HD + nb + PIECES, found, tail)
        return jnp.where(lane < HD + nb, (found - 1.0) * -masked, tail)

    def attend(load_tile, extra, causal, first):
        count = extra.shape[0]
        low = iota((count, LANES), 1) < HD
        for g in range(kv_heads):
            at = g * HD // LANES * LANES
            k = load_tile(at).astype(F32)
            v = load_tile(k_cols + at).astype(F32)
            if g % 2:
                k = pltpu.roll(k, HD, 1)
                v = pltpu.roll(v, HD, 1)
            k = jnp.where(low, k, extra).astype(BF16)
            v = jnp.where(low, v, 1.0).astype(BF16)
            for h in range(g * group, (g + 1) * group):
                weights = jnp.exp2(dot_nt(q_s[h], k))
                if causal is not None:
                    weights = jnp.where(causal, weights, 0.0)
                add = dot(weights.astype(BF16), v)
                if first:
                    acc[h] = add
                else:
                    acc[h] += add

    hot_own = jnp.where(
        iota((rows, nbp), 1) == me * nb + iota((rows, nbp), 0) // BLK, 1.0, 0.0).astype(BF16)
    causal = iota((rows, rows), 1) <= iota((rows, rows), 0)
    attend(lambda at: kv_s[:, at:at + LANES], key_extra(hot_own), causal, True)

    slot = (iota((picked, nbp), 0) // BLK).astype(F32)
    lane_owner = iota((picked, nbp), 1) // nb

    def absorb(d):
        @pl.when(me - d >= 0)
        def _():
            owner = lax.max(me - d, 0)
            hot = jnp.where((place[0:1] == slot) & (lane_owner == owner), 1.0, 0.0)
            extra = key_extra(hot.astype(BF16))
            kv_copy(owner, me, d).wait_recv()
            attend(lambda at: recv_s[owner, :, at:at + LANES], extra, None, False)

    peers(absorb)

    loads["wo0"].wait()
    loads["wo1"].wait()
    part_rows = rows // PARTS
    low = iota((part_rows, LANES), 1) < HD
    lane = iota((part_rows, LANES), 1)

    def part_copy(part):
        at = pl.ds(part * part_rows, part_rows)
        return pltpu.make_async_remote_copy(
            part_send.at[at], part_recv.at[at], part_sem.at[0, part], part_sem.at[1, part],
            device_id={"tp": partner}, device_id_type=pl.DeviceIdType.MESH)

    attended, all_sums = [], []
    for part in range(PARTS):
        at = slice(part * part_rows, (part + 1) * part_rows)
        sums = jnp.ones((part_rows, LANES), F32)
        tiles = []
        for tile in range(q_cols // LANES):
            pair = []
            for odd in range(2):
                head = 2 * tile + odd
                o = acc[head, at]
                total = pltpu.roll(o, HD, 1)
                sums = jnp.where(lane == head, total, sums)
                pair.append(o / total)
            tiles.append(jnp.where(low, pair[0], pltpu.roll(pair[1], HD, 1)))
        attended.append(jnp.concatenate(tiles, axis=1).astype(BF16))
        all_sums.append(sums)
        part_send[at] = dot(attended[part], wo_buf[1]).astype(BF16)
        part_copy(part).start()

    own = [dot(a, wo_buf[0]) for a in attended]
    logs = jnp.log(jnp.concatenate(all_sums, axis=0))
    logs = logs - slope_of(lane_q) * alibi * row_q.astype(F32)
    lt_ref[...] = logs.T[0:heads]

    def finish(d):
        @pl.when(me + d < n_kv)
        def _():
            kv_copy(me, lax.min(me + d, n_kv - 1), d).wait_send()

        @pl.when(me - d >= 0)
        def _():
            code_copy(me, lax.max(me - d, 0), d).wait_send()

    peers(finish)
    for part in range(PARTS):
        at = slice(part * part_rows, (part + 1) * part_rows)
        part_copy(part).wait()
        out_ref[at] = (own[part] + part_recv[at].astype(F32)).astype(BF16)


def write_out(mixed, log_total, mixed_out, log_out, sems):
    copies = [
        pltpu.make_async_copy(mixed, mixed_out, sems.at[0]),
        pltpu.make_async_copy(log_total, log_out, sems.at[1]),
    ]
    for copy in copies:
        copy.start()
    for copy in copies:
        copy.wait()


def shards(n_kv, tokens, norm_gain, w_query, w_key, w_value, q_gain, k_gain, w_out, chosen):
    seqs, rows, half = tokens.shape
    nb, entries = chosen.shape[1:]
    q_cols, k_cols = w_query.shape[1], w_key.shape[1]
    heads = q_cols // HD
    vmem = pltpu.VMEM
    dma = pltpu.SemaphoreType.DMA
    mixed, log_total = pl.pallas_call(
        functools.partial(kernel, n_kv),
        out_shape=(vmem((rows, half), BF16), vmem((heads, rows), F32)),
        in_specs=[pl.BlockSpec(memory_space=pltpu.HBM)] * 9,
        out_specs=(pl.BlockSpec(memory_space=vmem), pl.BlockSpec(memory_space=vmem)),
        scratch_shapes=[
            vmem((2, rows, half), BF16),
            vmem((nb, entries), jnp.int32),
            vmem((n_kv, 8, rows), F32),
            vmem((n_kv, 8, rows), F32),
            vmem((rows, q_cols + 2 * k_cols), F32),
            vmem((2, half, q_cols + 2 * k_cols), BF16),
            vmem((2, q_cols, half), BF16),
            vmem((2, 1, half), F32),
            vmem((1, HD), F32),
            vmem((1, HD), F32),
            vmem((heads, rows, LANES), BF16),
            vmem((rows, 2 * k_cols), BF16),
            vmem((n_kv, MOST * BLK, 2 * k_cols), BF16),
            vmem((n_kv, MOST * BLK, 2 * k_cols), BF16),
            vmem((heads, rows, LANES), F32),
            vmem((rows, half), BF16),
            vmem((rows, half), BF16),
            dma((14,)),
            dma((2,)),
            dma((2, n_kv)),
            dma((2, n_kv)),
            dma((2, PARTS)),
        ],
        compiler_params=pltpu.CompilerParams(
            collective_id=0, has_side_effects=True, vmem_limit_bytes=66_700_000
        ),
    )(
        tokens.reshape(rows, half), norm_gain.reshape(1, -1), w_query, w_key, w_value,
        q_gain.reshape(1, -1), k_gain.reshape(1, -1), w_out, chosen.reshape(nb, entries),
    )
    mixed, log_total = pl.pallas_call(
        write_out,
        out_shape=(
            jax.ShapeDtypeStruct((rows, half), BF16),
            jax.ShapeDtypeStruct((heads, rows), F32),
        ),
        in_specs=[pl.BlockSpec(memory_space=pl.ANY)] * 2,
        out_specs=(pl.BlockSpec(memory_space=pltpu.HBM),) * 2,
        scratch_shapes=[dma((2,))],
        compiler_params=pltpu.CompilerParams(vmem_limit_bytes=1_000_000),
    )(mixed, log_total)
    return mixed.reshape(seqs, rows, half), log_total.reshape(seqs, heads, rows)


def solution(mesh):
    in_specs = (
        P("dp", "kv", "tp"),
        P(),
        P(None, "tp"),
        P(None, "tp"),
        P(None, "tp"),
        P(),
        P(),
        P("tp", None),
        P("dp", "kv", None),
    )
    out_specs = (P("dp", "kv", "tp"), P("dp", "tp", "kv"))
    return jax.shard_map(
        functools.partial(shards, mesh.shape["kv"]),
        mesh=mesh, in_specs=in_specs, out_specs=out_specs, check_vma=False)
```

```python
import functools
import math

import jax
import jax.numpy as jnp
from jax import lax
from jax.experimental import pallas as pl
from jax.experimental.pallas import tpu as pltpu
from jax.sharding import PartitionSpec as P

HD = 64
BLK = 32
MOST = 4
LANES = 128
PIECES = 3
PARTS = 2

epsilon = 1e-06
alibi_reach = 4.0
masked = -1e30
LOG2E = math.log2(math.e)
F32 = jnp.float32
BF16 = jnp.bfloat16
NT = (((1,), (1,)), ((), ()))


def iota(shape, dim):
    return lax.broadcasted_iota(jnp.int32, shape, dim)


def dot(a, b):
    return jnp.dot(a, b, preferred_element_type=F32)


def dot_nt(a, b):
    return lax.dot_general(a, b, NT, preferred_element_type=F32)


def kernel(
    n_kv,
    tok, gain, wq, wk, wv, qg, kg, wo, ch,
    out_ref, lt_ref,
    x_buf, ch_buf, code_send, code_recv, raw_s, w_buf, wo_buf, g_buf, qg_buf, kg_buf,
    q_s, kv_s, send_s, recv_s, acc, part_send, part_recv,
    load_sem, x_sem, ch_sem, kv_sem, part_sem,
):
    me = lax.axis_index("kv")
    tp = lax.axis_index("tp")
    partner = 1 - tp
    rows, half = tok.shape
    q_cols = wq.shape[1]
    k_cols = wk.shape[1]
    heads = q_cols // HD
    kv_heads = k_cols // HD
    group = heads // kv_heads
    n_heads = heads * lax.axis_size("tp")
    nb = ch.shape[0]
    entries = ch.shape[1]
    nbp = -(-n_kv * nb // LANES) * LANES
    picked = MOST * BLK
    width = half * 2
    seq_len = rows * n_kv
    alibi = alibi_reach / seq_len

    def span(start):
        return pl.ds(pl.multiple_of(start * half, LANES), half)

    loads = {}

    def load(name, src, dst):
        copy = pltpu.make_async_copy(src, dst, load_sem.at[len(loads)])
        copy.start()
        loads[name] = copy

    sides = ((0, tp), (1, partner))
    load("ch", ch, ch_buf)
    load("tok", tok, x_buf.at[0])
    load("g0", gain.at[:, span(tp)], g_buf.at[0])
    for side, which in sides:
        load(f"wk{side}", wk.at[span(which), :], w_buf.at[side, :, q_cols:q_cols + k_cols])
        load(f"wv{side}", wv.at[span(which), :], w_buf.at[side, :, q_cols + k_cols:q_cols + 2 * k_cols])
        load(f"wq{side}", wq.at[span(which), :], w_buf.at[side, :, 0:q_cols])
    load("g1", gain.at[:, span(partner)], g_buf.at[1])
    load("qg", qg, qg_buf)
    load("kg", kg, kg_buf)
    for side, which in sides:
        load(f"wo{side}", wo.at[:, span(which)], wo_buf.at[side])

    def peers(step):
        if n_kv <= 8:
            for d in range(1, n_kv):
                step(d)
        else:
            lax.fori_loop(1, n_kv, lambda d, c: (step(d), c)[1], 0)

    def far_first(step):
        peers(lambda d: step(n_kv - d))

    barrier = pltpu.get_barrier_semaphore()
    pl.semaphore_signal(barrier, inc=1, device_id={"tp": partner}, device_id_type=pl.DeviceIdType.MESH)
    peers(lambda d: pl.semaphore_signal(
        barrier, inc=1, device_id={"kv": lax.rem(me + d, n_kv)}, device_id_type=pl.DeviceIdType.MESH))

    loads["ch"].wait()
    lane_block = iota((nb, nbp), 1)
    lists = ch_buf[...]
    hit = lists[:, 0:1] == lane_block
    for e in range(1, entries):
        hit = hit | (lists[:, e:e + 1] == lane_block)
    member = jnp.where(hit, 1.0, 0.0)
    before = jnp.where(
        (iota((nbp, nbp), 0) < iota((nbp, nbp), 1))
        & (iota((nbp, nbp), 0) // nb == iota((nbp, nbp), 1) // nb), 1.0, 0.0).astype(BF16)
    need = jnp.broadcast_to(jnp.max(member, axis=0, keepdims=True), (8, nbp))
    place = jnp.where(need > 0.5, dot(need.astype(BF16), before), -1.0)

    def place_rows(owner):
        spread = jnp.where(
            iota((nbp, rows), 0) == owner * nb + iota((nbp, rows), 1) // BLK, 1.0, 0.0)
        return dot(place.astype(BF16), spread.astype(BF16))

    def prepare_code(d):
        code_send[d] = place_rows(me - d)

    peers(prepare_code)

    def scaled(side):
        x = x_buf[side].astype(F32)
        return (x * g_buf[side]).astype(BF16), jnp.sum(x * x, axis=1, keepdims=True)

    for name in ("tok", "g0", "wk0", "wv0", "wq0"):
        loads[name].wait()
    y0, sq0 = scaled(0)
    raw_s[...] = dot(y0, w_buf[0])
    pl.semaphore_wait(barrier, n_kv)

    def code_copy(owner, target, d):
        return pltpu.make_async_remote_copy(
            code_send.at[d], code_recv.at[owner], ch_sem.at[0, target], ch_sem.at[1, owner],
            device_id={"kv": target}, device_id_type=pl.DeviceIdType.MESH)

    def send_code(d):
        @pl.when(me - d >= 0)
        def _():
            code_copy(me, lax.max(me - d, 0), d).start()

    peers(send_code)

    x_copy = pltpu.make_async_remote_copy(
        x_buf.at[0], x_buf.at[1], x_sem.at[0], x_sem.at[1],
        device_id={"tp": partner}, device_id_type=pl.DeviceIdType.MESH)
    x_copy.start()

    same_head = jnp.where(
        iota((LANES, LANES), 0) // HD == iota((LANES, LANES), 1) // HD, 1.0, 0.0).astype(BF16)

    def head_norm(v, gain_row):
        sq = v * v
        hi = sq.astype(BF16)
        lo = (sq - hi.astype(F32)).astype(BF16)
        total = dot(hi, same_head) + dot(lo, same_head)
        return v * lax.rsqrt(total / HD + epsilon) * gain_row

    for name in ("g1", "qg", "kg", "wk1", "wv1", "wq1"):
        loads[name].wait()
    qg_row = jnp.concatenate([qg_buf[...], qg_buf[...]], axis=1) * (HD ** -0.5 * LOG2E)
    kg_row = jnp.concatenate([kg_buf[...], kg_buf[...]], axis=1)
    x_copy.wait()
    y1, sq1 = scaled(1)
    row_scale = lax.rsqrt((sq0 + sq1) / width + epsilon)
    raw_kv = (raw_s[:, q_cols:] + dot(y1, w_buf[1, :, q_cols:])) * row_scale
    for tile in range(k_cols // LANES):
        at = tile * LANES
        kv_s[:, at:at + LANES] = head_norm(raw_kv[:, at:at + LANES], kg_row).astype(BF16)
    kv_s[:, k_cols:] = raw_kv[:, k_cols:].astype(BF16)

    same_row = iota((picked, rows), 0) % BLK == iota((picked, rows), 1) % BLK
    row_slot = (iota((picked, rows), 0) // BLK).astype(F32)

    def kv_copy(owner, target, d):
        return pltpu.make_async_remote_copy(
            send_s.at[d], recv_s.at[owner], kv_sem.at[0, target], kv_sem.at[1, owner],
            device_id={"kv": target}, device_id_type=pl.DeviceIdType.MESH)

    def send_rows(d):
        @pl.when(me + d < n_kv)
        def _():
            target = lax.min(me + d, n_kv - 1)
            code_copy(target, me, d).wait_recv()
            code = code_recv[target][0:1]
            chosen_rows = jnp.where(same_row & (code == row_slot), 1.0, 0.0).astype(BF16)
            send_s[d] = dot(chosen_rows, kv_s[...]).astype(BF16)
            kv_copy(me, target, d).start()

    far_first(send_rows)
    raw = (raw_s[:, 0:q_cols] + dot(y1, w_buf[1, :, 0:q_cols])) * row_scale

    lane_q = iota((rows, LANES), 1)
    row_q = iota((rows, LANES), 0)
    own_block = jnp.where(lane_q - HD == row_q // BLK, 1.0, 0.0)

    def slope_of(head):
        return jnp.exp2(-8.0 / n_heads * (tp * heads + head + 1).astype(F32))

    def lane_fill(base, first, value):
        return jnp.where(lane_q == first, value, base)

    for tile in range(q_cols // LANES):
        at = tile * LANES
        q = head_norm(raw[:, at:at + LANES], qg_row)
        for odd in range(2):
            head = 2 * tile + odd
            value = slope_of(jnp.full((rows, LANES), head, jnp.int32)) * (alibi * LOG2E)
            extra = own_block
            for piece in range(PIECES):
                part = value.astype(BF16).astype(F32)
                value = value - part
                extra = lane_fill(extra, HD + nb + piece, part * BLK)
                extra = lane_fill(extra, HD + nb + PIECES + piece, part)
            here = q if odd == 0 else pltpu.roll(q, HD, 1)
            q_s[head] = jnp.where(lane_q < HD, here, extra).astype(BF16)

    relative = (lane_block - me * nb).astype(F32)
    pieces_rows = jnp.where(
        iota((8, nbp), 0) < PIECES,
        jnp.broadcast_to(relative[0:1], (8, nbp)), 0.0)
    table = jnp.concatenate(
        [jnp.zeros((HD, nbp), F32), member, pieces_rows,
         jnp.zeros((LANES - HD - nb - 8, nbp), F32)], axis=0).astype(BF16)

    def key_extra(hot):
        count = hot.shape[0]
        lane = iota((count, LANES), 1)
        found = dot_nt(hot, table)
        inside = (iota((count, LANES), 0) % BLK).astype(F32)
        tail = jnp.where(lane < HD + nb + 2 * PIECES, inside, 0.0)
        tail = jnp.where(lane < HD + nb + PIECES, found, tail)
        return jnp.where(lane < HD + nb, (found - 1.0) * -masked, tail)

    def attend(load_tile, extra, causal, first):
        count = extra.shape[0]
        low = iota((count, LANES), 1) < HD
        for g in range(kv_heads):
            at = g * HD // LANES * LANES
            k = load_tile(at).astype(F32)
            v = load_tile(k_cols + at).astype(F32)
            if g % 2:
                k = pltpu.roll(k, HD, 1)
                v = pltpu.roll(v, HD, 1)
            k = jnp.where(low, k, extra).astype(BF16)
            v = jnp.where(low, v, 1.0).astype(BF16)
            for h in range(g * group, (g + 1) * group):
                weights = jnp.exp2(dot_nt(q_s[h], k))
                if causal is not None:
                    weights = jnp.where(causal, weights, 0.0)
                add = dot(weights.astype(BF16), v)
                if first:
                    acc[h] = add
                else:
                    acc[h] += add

    hot_own = jnp.where(
        iota((rows, nbp), 1) == me * nb + iota((rows, nbp), 0) // BLK, 1.0, 0.0).astype(BF16)
    causal = iota((rows, rows), 1) <= iota((rows, rows), 0)
    attend(lambda at: kv_s[:, at:at + LANES], key_extra(hot_own), causal, True)

    slot = (iota((picked, nbp), 0) // BLK).astype(F32)
    lane_owner = iota((picked, nbp), 1) // nb

    def absorb(d):
        @pl.when(me - d >= 0)
        def _():
            owner = lax.max(me - d, 0)
            hot = jnp.where((place[0:1] == slot) & (lane_owner == owner), 1.0, 0.0)
            extra = key_extra(hot.astype(BF16))
            kv_copy(owner, me, d).wait_recv()
            attend(lambda at: recv_s[owner, :, at:at + LANES], extra, None, False)

    far_first(absorb)

    loads["wo0"].wait()
    loads["wo1"].wait()
    part_rows = rows // PARTS
    low = iota((part_rows, LANES), 1) < HD
    lane = iota((part_rows, LANES), 1)

    def part_copy(part):
        at = pl.ds(part * part_rows, part_rows)
        return pltpu.make_async_remote_copy(
            part_send.at[at], part_recv.at[at], part_sem.at[0, part], part_sem.at[1, part],
            device_id={"tp": partner}, device_id_type=pl.DeviceIdType.MESH)

    attended, all_sums = [], []
    for part in range(PARTS):
        at = slice(part * part_rows, (part + 1) * part_rows)
        sums = jnp.ones((part_rows, LANES), F32)
        tiles = []
        for tile in range(q_cols // LANES):
            pair = []
            for odd in range(2):
                pair.append(acc[2 * tile + odd, at])
            turned = [pltpu.roll(o, HD, 1) for o in pair]
            total = jnp.where(low, turned[0], pair[1])
            tiles.append(jnp.where(low, pair[0], turned[1]) / total)
            for odd in range(2):
                sums = jnp.where(lane == 2 * tile + odd, turned[odd], sums)
        attended.append(jnp.concatenate(tiles, axis=1).astype(BF16))
        all_sums.append(sums)
        part_send[at] = dot(attended[part], wo_buf[1]).astype(BF16)
        part_copy(part).start()

    own = [dot(a, wo_buf[0]) for a in attended]
    logs = jnp.log(jnp.concatenate(all_sums, axis=0))
    logs = logs - slope_of(lane_q) * alibi * row_q.astype(F32)
    lt_ref[...] = logs.T[0:heads]

    def finish(d):
        @pl.when(me + d < n_kv)
        def _():
            kv_copy(me, lax.min(me + d, n_kv - 1), d).wait_send()

        @pl.when(me - d >= 0)
        def _():
            code_copy(me, lax.max(me - d, 0), d).wait_send()

    peers(finish)
    for part in range(PARTS):
        at = slice(part * part_rows, (part + 1) * part_rows)
        part_copy(part).wait()
        out_ref[at] = (own[part] + part_recv[at].astype(F32)).astype(BF16)


def write_out(mixed, log_total, mixed_out, log_out, sems):
    copies = [
        pltpu.make_async_copy(mixed, mixed_out, sems.at[0]),
        pltpu.make_async_copy(log_total, log_out, sems.at[1]),
    ]
    for copy in copies:
        copy.start()
    for copy in copies:
        copy.wait()


def shards(n_kv, tokens, norm_gain, w_query, w_key, w_value, q_gain, k_gain, w_out, chosen):
    seqs, rows, half = tokens.shape
    nb, entries = chosen.shape[1:]
    q_cols, k_cols = w_query.shape[1], w_key.shape[1]
    heads = q_cols // HD
    vmem = pltpu.VMEM
    dma = pltpu.SemaphoreType.DMA
    mixed, log_total = pl.pallas_call(
        functools.partial(kernel, n_kv),
        out_shape=(vmem((rows, half), BF16), vmem((heads, rows), F32)),
        in_specs=[pl.BlockSpec(memory_space=pltpu.HBM)] * 9,
        out_specs=(pl.BlockSpec(memory_space=vmem), pl.BlockSpec(memory_space=vmem)),
        scratch_shapes=[
            vmem((2, rows, half), BF16),
            vmem((nb, entries), jnp.int32),
            vmem((n_kv, 8, rows), F32),
            vmem((n_kv, 8, rows), F32),
            vmem((rows, q_cols + 2 * k_cols), F32),
            vmem((2, half, q_cols + 2 * k_cols), BF16),
            vmem((2, q_cols, half), BF16),
            vmem((2, 1, half), F32),
            vmem((1, HD), F32),
            vmem((1, HD), F32),
            vmem((heads, rows, LANES), BF16),
            vmem((rows, 2 * k_cols), BF16),
            vmem((n_kv, MOST * BLK, 2 * k_cols), BF16),
            vmem((n_kv, MOST * BLK, 2 * k_cols), BF16),
            vmem((heads, rows, LANES), F32),
            vmem((rows, half), BF16),
            vmem((rows, half), BF16),
            dma((14,)),
            dma((2,)),
            dma((2, n_kv)),
            dma((2, n_kv)),
            dma((2, PARTS)),
        ],
        compiler_params=pltpu.CompilerParams(
            collective_id=0, has_side_effects=True, vmem_limit_bytes=66_700_000
        ),
    )(
        tokens.reshape(rows, half), norm_gain.reshape(1, -1), w_query, w_key, w_value,
        q_gain.reshape(1, -1), k_gain.reshape(1, -1), w_out, chosen.reshape(nb, entries),
    )
    mixed, log_total = pl.pallas_call(
        write_out,
        out_shape=(
            jax.ShapeDtypeStruct((rows, half), BF16),
            jax.ShapeDtypeStruct((heads, rows), F32),
        ),
        in_specs=[pl.BlockSpec(memory_space=pl.ANY)] * 2,
        out_specs=(pl.BlockSpec(memory_space=pltpu.HBM),) * 2,
        scratch_shapes=[dma((2,))],
        compiler_params=pltpu.CompilerParams(vmem_limit_bytes=1_000_000),
    )(mixed, log_total)
    return mixed.reshape(seqs, rows, half), log_total.reshape(seqs, heads, rows)


def solution(mesh):
    in_specs = (
        P("dp", "kv", "tp"),
        P(),
        P(None, "tp"),
        P(None, "tp"),
        P(None, "tp"),
        P(),
        P(),
        P("tp", None),
        P("dp", "kv", None),
    )
    out_specs = (P("dp", "kv", "tp"), P("dp", "tp", "kv"))
    return jax.shard_map(
        functools.partial(shards, mesh.shape["kv"]),
        mesh=mesh, in_specs=in_specs, out_specs=out_specs, check_vma=False)
```

```python
import functools
import math

import jax
import jax.numpy as jnp
from jax import lax
from jax.experimental import pallas as pl
from jax.experimental.pallas import tpu as pltpu
from jax.sharding import PartitionSpec as P

HD = 64
BLK = 32
MOST = 4
LANES = 128
PIECES = 3
PARTS = 2

epsilon = 1e-06
alibi_reach = 4.0
masked = -1e30
LOG2E = math.log2(math.e)
F32 = jnp.float32
BF16 = jnp.bfloat16
NT = (((1,), (1,)), ((), ()))


def iota(shape, dim):
    return lax.broadcasted_iota(jnp.int32, shape, dim)


def dot(a, b):
    return jnp.dot(a, b, preferred_element_type=F32)


def dot_nt(a, b):
    return lax.dot_general(a, b, NT, preferred_element_type=F32)


def kernel(
    n_kv,
    tok, gain, wq, wk, wv, qg, kg, wo, ch,
    out_ref, lt_ref,
    x_buf, ch_buf, code_send, code_recv, raw_s, w_buf, wo_buf, g_buf, qg_buf, kg_buf,
    q_s, kv_s, send_s, recv_s, acc, part_send, part_recv,
    load_sem, x_sem, ch_sem, kv_sem, part_sem,
):
    me = lax.axis_index("kv")
    tp = lax.axis_index("tp")
    partner = 1 - tp
    rows, half = tok.shape
    q_cols = wq.shape[1]
    k_cols = wk.shape[1]
    heads = q_cols // HD
    kv_heads = k_cols // HD
    group = heads // kv_heads
    n_heads = heads * lax.axis_size("tp")
    nb = ch.shape[0]
    entries = ch.shape[1]
    nbp = -(-n_kv * nb // LANES) * LANES
    picked = MOST * BLK
    width = half * 2
    seq_len = rows * n_kv
    alibi = alibi_reach / seq_len

    def span(start):
        return pl.ds(pl.multiple_of(start * half, LANES), half)

    loads = {}

    def load(name, src, dst):
        copy = pltpu.make_async_copy(src, dst, load_sem.at[len(loads)])
        copy.start()
        loads[name] = copy

    sides = ((0, tp), (1, partner))
    load("ch", ch, ch_buf)
    load("tok", tok, x_buf.at[0])
    load("g0", gain.at[:, span(tp)], g_buf.at[0])
    for side, which in sides:
        load(f"wk{side}", wk.at[span(which), :], w_buf.at[side, :, q_cols:q_cols + k_cols])
        load(f"wv{side}", wv.at[span(which), :], w_buf.at[side, :, q_cols + k_cols:q_cols + 2 * k_cols])
        load(f"wq{side}", wq.at[span(which), :], w_buf.at[side, :, 0:q_cols])
    load("g1", gain.at[:, span(partner)], g_buf.at[1])
    load("qg", qg, qg_buf)
    load("kg", kg, kg_buf)
    for side, which in sides:
        load(f"wo{side}", wo.at[:, span(which)], wo_buf.at[side])

    def peers(step):
        if n_kv <= 8:
            for d in range(1, n_kv):
                step(d)
        else:
            lax.fori_loop(1, n_kv, lambda d, c: (step(d), c)[1], 0)

    def far_first(step):
        peers(lambda d: step(n_kv - d))

    barrier = pltpu.get_barrier_semaphore()
    pl.semaphore_signal(barrier, inc=1, device_id={"tp": partner}, device_id_type=pl.DeviceIdType.MESH)
    peers(lambda d: pl.semaphore_signal(
        barrier, inc=1, device_id={"kv": lax.rem(me + d, n_kv)}, device_id_type=pl.DeviceIdType.MESH))

    loads["ch"].wait()
    lane_block = iota((nb, nbp), 1)
    lists = ch_buf[...]
    hit = lists[:, 0:1] == lane_block
    for e in range(1, entries):
        hit = hit | (lists[:, e:e + 1] == lane_block)
    member = jnp.where(hit, 1.0, 0.0)
    before = jnp.where(
        (iota((nbp, nbp), 0) < iota((nbp, nbp), 1))
        & (iota((nbp, nbp), 0) // nb == iota((nbp, nbp), 1) // nb), 1.0, 0.0).astype(BF16)
    need = jnp.broadcast_to(jnp.max(member, axis=0, keepdims=True), (8, nbp))
    place = jnp.where(need > 0.5, dot(need.astype(BF16), before), -1.0)

    def place_rows(owner):
        spread = jnp.where(
            iota((nbp, rows), 0) == owner * nb + iota((nbp, rows), 1) // BLK, 1.0, 0.0)
        return dot(place.astype(BF16), spread.astype(BF16))

    def prepare_code(d):
        code_send[d] = place_rows(me - d)

    peers(prepare_code)

    def scaled(side):
        x = x_buf[side].astype(F32)
        return (x * g_buf[side]).astype(BF16), jnp.sum(x * x, axis=1, keepdims=True)

    for name in ("tok", "g0", "wk0", "wv0", "wq0"):
        loads[name].wait()
    y0, sq0 = scaled(0)
    raw_s[:, q_cols:] = dot(y0, w_buf[0, :, q_cols:])
    pl.semaphore_wait(barrier, n_kv)

    def code_copy(owner, target, d):
        return pltpu.make_async_remote_copy(
            code_send.at[d], code_recv.at[owner], ch_sem.at[0, target], ch_sem.at[1, owner],
            device_id={"kv": target}, device_id_type=pl.DeviceIdType.MESH)

    def send_code(d):
        @pl.when(me - d >= 0)
        def _():
            code_copy(me, lax.max(me - d, 0), d).start()

    peers(send_code)

    x_copy = pltpu.make_async_remote_copy(
        x_buf.at[0], x_buf.at[1], x_sem.at[0], x_sem.at[1],
        device_id={"tp": partner}, device_id_type=pl.DeviceIdType.MESH)
    x_copy.start()

    same_head = jnp.where(
        iota((LANES, LANES), 0) // HD == iota((LANES, LANES), 1) // HD, 1.0, 0.0).astype(BF16)

    def head_norm(v, gain_row):
        sq = v * v
        hi = sq.astype(BF16)
        lo = (sq - hi.astype(F32)).astype(BF16)
        total = dot(hi, same_head) + dot(lo, same_head)
        return v * lax.rsqrt(total / HD + epsilon) * gain_row

    for name in ("g1", "qg", "kg", "wk1", "wv1", "wq1"):
        loads[name].wait()
    qg_row = jnp.concatenate([qg_buf[...], qg_buf[...]], axis=1) * (HD ** -0.5 * LOG2E)
    kg_row = jnp.concatenate([kg_buf[...], kg_buf[...]], axis=1)
    x_copy.wait()
    y1, sq1 = scaled(1)
    row_scale = lax.rsqrt((sq0 + sq1) / width + epsilon)
    raw_kv = (raw_s[:, q_cols:] + dot(y1, w_buf[1, :, q_cols:])) * row_scale
    for tile in range(k_cols // LANES):
        at = tile * LANES
        kv_s[:, at:at + LANES] = head_norm(raw_kv[:, at:at + LANES], kg_row).astype(BF16)
    kv_s[:, k_cols:] = raw_kv[:, k_cols:].astype(BF16)

    same_row = iota((picked, rows), 0) % BLK == iota((picked, rows), 1) % BLK
    row_slot = (iota((picked, rows), 0) // BLK).astype(F32)

    def kv_copy(owner, target, d):
        return pltpu.make_async_remote_copy(
            send_s.at[d], recv_s.at[owner], kv_sem.at[0, target], kv_sem.at[1, owner],
            device_id={"kv": target}, device_id_type=pl.DeviceIdType.MESH)

    def send_rows(d):
        @pl.when(me + d < n_kv)
        def _():
            target = lax.min(me + d, n_kv - 1)
            code_copy(target, me, d).wait_recv()
            code = code_recv[target][0:1]
            chosen_rows = jnp.where(same_row & (code == row_slot), 1.0, 0.0).astype(BF16)
            send_s[d] = dot(chosen_rows, kv_s[...]).astype(BF16)
            kv_copy(me, target, d).start()

    far_first(send_rows)
    raw = (dot(y0, w_buf[0, :, 0:q_cols]) + dot(y1, w_buf[1, :, 0:q_cols])) * row_scale

    lane_q = iota((rows, LANES), 1)
    row_q = iota((rows, LANES), 0)
    own_block = jnp.where(lane_q - HD == row_q // BLK, 1.0, 0.0)

    def slope_of(head):
        return jnp.exp2(-8.0 / n_heads * (tp * heads + head + 1).astype(F32))

    def lane_fill(base, first, value):
        return jnp.where(lane_q == first, value, base)

    for tile in range(q_cols // LANES):
        at = tile * LANES
        q = head_norm(raw[:, at:at + LANES], qg_row)
        for odd in range(2):
            head = 2 * tile + odd
            value = slope_of(jnp.full((rows, LANES), head, jnp.int32)) * (alibi * LOG2E)
            extra = own_block
            for piece in range(PIECES):
                part = value.astype(BF16).astype(F32)
                value = value - part
                extra = lane_fill(extra, HD + nb + piece, part * BLK)
                extra = lane_fill(extra, HD + nb + PIECES + piece, part)
            here = q if odd == 0 else pltpu.roll(q, HD, 1)
            q_s[head] = jnp.where(lane_q < HD, here, extra).astype(BF16)

    relative = (lane_block - me * nb).astype(F32)
    pieces_rows = jnp.where(
        iota((8, nbp), 0) < PIECES,
        jnp.broadcast_to(relative[0:1], (8, nbp)), 0.0)
    table = jnp.concatenate(
        [jnp.zeros((HD, nbp), F32), member, pieces_rows,
         jnp.zeros((LANES - HD - nb - 8, nbp), F32)], axis=0).astype(BF16)

    def key_extra(hot):
        count = hot.shape[0]
        lane = iota((count, LANES), 1)
        found = dot_nt(hot, table)
        inside = (iota((count, LANES), 0) % BLK).astype(F32)
        tail = jnp.where(lane < HD + nb + 2 * PIECES, inside, 0.0)
        tail = jnp.where(lane < HD + nb + PIECES, found, tail)
        return jnp.where(lane < HD + nb, (found - 1.0) * -masked, tail)

    def attend(load_tile, extra, causal, first):
        count = extra.shape[0]
        low = iota((count, LANES), 1) < HD
        for g in range(kv_heads):
            at = g * HD // LANES * LANES
            k = load_tile(at).astype(F32)
            v = load_tile(k_cols + at).astype(F32)
            if g % 2:
                k = pltpu.roll(k, HD, 1)
                v = pltpu.roll(v, HD, 1)
            k = jnp.where(low, k, extra).astype(BF16)
            v = jnp.where(low, v, 1.0).astype(BF16)
            for h in range(g * group, (g + 1) * group):
                weights = jnp.exp2(dot_nt(q_s[h], k))
                if causal is not None:
                    weights = jnp.where(causal, weights, 0.0)
                add = dot(weights.astype(BF16), v)
                if first:
                    acc[h] = add
                else:
                    acc[h] += add

    hot_own = jnp.where(
        iota((rows, nbp), 1) == me * nb + iota((rows, nbp), 0) // BLK, 1.0, 0.0).astype(BF16)
    causal = iota((rows, rows), 1) <= iota((rows, rows), 0)
    attend(lambda at: kv_s[:, at:at + LANES], key_extra(hot_own), causal, True)

    slot = (iota((picked, nbp), 0) // BLK).astype(F32)
    lane_owner = iota((picked, nbp), 1) // nb

    def absorb(d):
        @pl.when(me - d >= 0)
        def _():
            owner = lax.max(me - d, 0)
            hot = jnp.where((place[0:1] == slot) & (lane_owner == owner), 1.0, 0.0)
            extra = key_extra(hot.astype(BF16))
            kv_copy(owner, me, d).wait_recv()
            attend(lambda at: recv_s[owner, :, at:at + LANES], extra, None, False)

    far_first(absorb)

    loads["wo0"].wait()
    loads["wo1"].wait()
    part_rows = rows // PARTS
    low = iota((part_rows, LANES), 1) < HD
    lane = iota((part_rows, LANES), 1)

    def part_copy(part):
        at = pl.ds(part * part_rows, part_rows)
        return pltpu.make_async_remote_copy(
            part_send.at[at], part_recv.at[at], part_sem.at[0, part], part_sem.at[1, part],
            device_id={"tp": partner}, device_id_type=pl.DeviceIdType.MESH)

    attended, all_sums = [], []
    for part in range(PARTS):
        at = slice(part * part_rows, (part + 1) * part_rows)
        sums = jnp.ones((part_rows, LANES), F32)
        tiles = []
        for tile in range(q_cols // LANES):
            pair = []
            for odd in range(2):
                pair.append(acc[2 * tile + odd, at])
            turned = [pltpu.roll(o, HD, 1) for o in pair]
            total = jnp.where(low, turned[0], pair[1])
            tiles.append(jnp.where(low, pair[0], turned[1]) / total)
            for odd in range(2):
                sums = jnp.where(lane == 2 * tile + odd, turned[odd], sums)
        attended.append(jnp.concatenate(tiles, axis=1).astype(BF16))
        all_sums.append(sums)
        part_send[at] = dot(attended[part], wo_buf[1]).astype(BF16)
        part_copy(part).start()

    own = [dot(a, wo_buf[0]) for a in attended]
    logs = jnp.log(jnp.concatenate(all_sums, axis=0))
    logs = logs - slope_of(lane_q) * alibi * row_q.astype(F32)
    lt_ref[...] = logs.T[0:heads]

    def finish(d):
        @pl.when(me + d < n_kv)
        def _():
            kv_copy(me, lax.min(me + d, n_kv - 1), d).wait_send()

        @pl.when(me - d >= 0)
        def _():
            code_copy(me, lax.max(me - d, 0), d).wait_send()

    for part in range(PARTS):
        at = slice(part * part_rows, (part + 1) * part_rows)
        part_copy(part).wait()
        out_ref[at] = (own[part] + part_recv[at].astype(F32)).astype(BF16)
    peers(finish)


def write_out(mixed, log_total, mixed_out, log_out, sems):
    copies = [
        pltpu.make_async_copy(mixed, mixed_out, sems.at[0]),
        pltpu.make_async_copy(log_total, log_out, sems.at[1]),
    ]
    for copy in copies:
        copy.start()
    for copy in copies:
        copy.wait()


def shards(n_kv, tokens, norm_gain, w_query, w_key, w_value, q_gain, k_gain, w_out, chosen):
    seqs, rows, half = tokens.shape
    nb, entries = chosen.shape[1:]
    q_cols, k_cols = w_query.shape[1], w_key.shape[1]
    heads = q_cols // HD
    vmem = pltpu.VMEM
    dma = pltpu.SemaphoreType.DMA
    mixed, log_total = pl.pallas_call(
        functools.partial(kernel, n_kv),
        out_shape=(vmem((rows, half), BF16), vmem((heads, rows), F32)),
        in_specs=[pl.BlockSpec(memory_space=pltpu.HBM)] * 9,
        out_specs=(pl.BlockSpec(memory_space=vmem), pl.BlockSpec(memory_space=vmem)),
        scratch_shapes=[
            vmem((2, rows, half), BF16),
            vmem((nb, entries), jnp.int32),
            vmem((n_kv, 8, rows), F32),
            vmem((n_kv, 8, rows), F32),
            vmem((rows, q_cols + 2 * k_cols), F32),
            vmem((2, half, q_cols + 2 * k_cols), BF16),
            vmem((2, q_cols, half), BF16),
            vmem((2, 1, half), F32),
            vmem((1, HD), F32),
            vmem((1, HD), F32),
            vmem((heads, rows, LANES), BF16),
            vmem((rows, 2 * k_cols), BF16),
            vmem((n_kv, MOST * BLK, 2 * k_cols), BF16),
            vmem((n_kv, MOST * BLK, 2 * k_cols), BF16),
            vmem((heads, rows, LANES), F32),
            vmem((rows, half), BF16),
            vmem((rows, half), BF16),
            dma((14,)),
            dma((2,)),
            dma((2, n_kv)),
            dma((2, n_kv)),
            dma((2, PARTS)),
        ],
        compiler_params=pltpu.CompilerParams(
            collective_id=0, has_side_effects=True, vmem_limit_bytes=66_700_000
        ),
    )(
        tokens.reshape(rows, half), norm_gain.reshape(1, -1), w_query, w_key, w_value,
        q_gain.reshape(1, -1), k_gain.reshape(1, -1), w_out, chosen.reshape(nb, entries),
    )
    mixed, log_total = pl.pallas_call(
        write_out,
        out_shape=(
            jax.ShapeDtypeStruct((rows, half), BF16),
            jax.ShapeDtypeStruct((heads, rows), F32),
        ),
        in_specs=[pl.BlockSpec(memory_space=pl.ANY)] * 2,
        out_specs=(pl.BlockSpec(memory_space=pltpu.HBM),) * 2,
        scratch_shapes=[dma((2,))],
        compiler_params=pltpu.CompilerParams(vmem_limit_bytes=1_000_000),
    )(mixed, log_total)
    return mixed.reshape(seqs, rows, half), log_total.reshape(seqs, heads, rows)


def solution(mesh):
    in_specs = (
        P("dp", "kv", "tp"),
        P(),
        P(None, "tp"),
        P(None, "tp"),
        P(None, "tp"),
        P(),
        P(),
        P("tp", None),
        P("dp", "kv", None),
    )
    out_specs = (P("dp", "kv", "tp"), P("dp", "tp", "kv"))
    return jax.shard_map(
        functools.partial(shards, mesh.shape["kv"]),
        mesh=mesh, in_specs=in_specs, out_specs=out_specs, check_vma=False)
```
